32 devices in a mesh: grp: 2 (over y), fs: 4 (over z), tp: 4 (over x, core).
Axes of the slice: x: 2, y: 2, z: 4, core: 2. Of those that a mesh axis runs over, the one named last changes fastest.
Arguments:
- tokens: bfloat16 [3072, 2048], P(('grp', 'fs'), 'tp'), parts along dimension 0, may hold values from -25 to 25
- gain_first: float32 [2048], replicated, may hold values from 0.1 to 1.9
- gate_first: bfloat16 [2048, 5120], P('fs', 'tp'), may hold values from -0.125 to 0.125
- up_first: bfloat16 [2048, 5120], P('fs', 'tp'), may hold values from -0.125 to 0.125
- down_first: bfloat16 [5120, 2048], P('tp', 'fs'), may hold values from -0.078125 to 0.078125
- gain_mixer: float32 [2048], replicated, may hold values from 0.1 to 1.9
- outer_gate: bfloat16 [2048, 1024], P('fs', 'tp'), may hold values from -0.125 to 0.125
- inner_gate: bfloat16 [2048, 1024], P('fs', 'tp'), may hold values from -0.125 to 0.125
- conv_input: bfloat16 [2048, 1024], P('fs', 'tp'), may hold values from -0.125 to 0.125
- conv_taps: float32 [3, 1024], P(None, 'tp'), may hold values from -3.5 to 3.5
- mixer_out: bfloat16 [1024, 2048], P('tp', 'fs'), may hold values from -0.1875 to 0.1875
- gain_last: float32 [2048], replicated, may hold values from 0.1 to 1.9
- gate_last: bfloat16 [2048, 5120], P('fs', 'tp'), may hold values from -0.125 to 0.125
- up_last: bfloat16 [2048, 5120], P('fs', 'tp'), may hold values from -0.125 to 0.125
- down_last: bfloat16 [5120, 2048], P('tp', 'fs'), may hold values from -0.078125 to 0.078125
Outputs:
- layer_out: bfloat16 [3072, 2048], P(('grp', 'fs'), 'tp'), parts along dimension 0
The draws below stay inside these ranges and needn't reach their ends.
There are 2 independent parts, one for each index of `grp`. The reference program is written for one: setup_inputs(seed, part) draws one part's arguments, and reference() takes and returns one part's arrays. A program takes and returns all parts, laid end to end along the dimension named above; an argument that names none is the same for every part. Nothing has to cross between parts.
All inputs are finite; a program needn't handle non-finite values.
Results may differ from the reference program's by a relative error of at most 0.015.
Values may be sent and summed in bfloat16 or wider, within the bound.
No kernel may reach another device: no remote copies, remote signals or barrier semaphores. Data moves between devices by JAX's collectives and lax.ppermute only.
A program may use at most 64 MiB of HBM per device.

```python
import math
import jax
import jax.numpy as jnp
from jax import lax

D = 2048
FF = 5120
SC = 1024
KERNEL = 3
SEQ_LEN = 64
TOKENS = 1536
N_TP = 4


def draw_tokens(key, part):
    row_count = TOKENS
    col_count = D
    key_base, key_row, key_col = jax.random.split(jax.random.fold_in(key, 11), 3)
    values_raw = jnp.clip(jax.random.normal(key_base, (row_count, col_count), jnp.float32), -4.0, 4.0)
    row_scale = jnp.exp(jax.random.uniform(key_row, (row_count, 1), jnp.float32, math.log(0.5), math.log(2.0)))
    rising = 0.5 * jnp.power(4.0, jnp.arange(col_count, dtype=jnp.float32) / col_count)
    jitter = jnp.exp(jax.random.uniform(key_col, (col_count,), jnp.float32, -0.4, 0.4))
    return (values_raw * row_scale * (rising * jitter)[None, :]).astype(jnp.bfloat16)


def block_levels(key, shape, cuts, smallest, top_value):
    loudness = 1.0
    for position, shards_of in cuts:
        draws = jax.random.uniform(jax.random.fold_in(jax.random.fold_in(key, 6), position), (shards_of,), jnp.float32, smallest / len(cuts), top_value / len(cuts))
        loudness = loudness * jnp.repeat(jnp.exp(draws), shape[position] // shards_of).reshape((-1,) + (1,) * (len(shape) - 1 - position))
    return loudness


def scatter_about(key, shape, spread, limit, pieces=(), kind=jnp.bfloat16):
    drawn = spread * jax.random.normal(key, shape, jnp.float32)
    if pieces:
        drawn = drawn * block_levels(key, shape, pieces, -0.22, 0.18)
    return jnp.clip(drawn, -limit, limit).astype(kind)


def setup_inputs(seed: int = 0, part: int = 0) -> dict:
    key_of = jax.random.split(jax.random.key(seed), 16)
    part_keys = jax.random.split(jax.random.fold_in(key_of[15], part), 16)
    tokens = draw_tokens(jax.random.fold_in(jax.random.fold_in(key_of[15], part), 71), part)
    gain_first = jnp.clip(1.0 + 0.18 * jax.random.normal(key_of[1], (D,), jnp.float32), 0.1, 1.9)
    gate_first = scatter_about(key_of[2], (D, FF), D ** -0.5, 0.125, ((0, 4), (1, 4)))
    up_first = scatter_about(key_of[3], (D, FF), D ** -0.5, 0.125, ((0, 4), (1, 4)))
    down_first = scatter_about(key_of[4], (FF, D), FF ** -0.5, 0.078125, ((0, 4), (1, 4)))
    gain_mixer = jnp.clip(1.0 + 0.18 * jax.random.normal(key_of[5], (D,), jnp.float32), 0.1, 1.9)
    outer_gate = scatter_about(key_of[6], (D, SC), D ** -0.5, 0.125, ((0, 4), (1, 4)))
    inner_gate = scatter_about(key_of[7], (D, SC), D ** -0.5, 0.125, ((0, 4), (1, 4)))
    conv_input = scatter_about(key_of[8], (D, SC), D ** -0.5, 0.125, ((0, 4), (1, 4)))
    conv_taps = scatter_about(key_of[9], (KERNEL, SC), KERNEL ** -0.5, 3.5, ((1, 4),), jnp.float32)
    mixer_out = scatter_about(key_of[10], (SC, D), SC ** -0.5, 0.1875, ((0, 4), (1, 4)))
    gain_last = jnp.clip(1.0 + 0.18 * jax.random.normal(key_of[11], (D,), jnp.float32), 0.1, 1.9)
    gate_last = scatter_about(key_of[12], (D, FF), D ** -0.5, 0.125, ((0, 4), (1, 4)))
    up_last = scatter_about(key_of[13], (D, FF), D ** -0.5, 0.125, ((0, 4), (1, 4)))
    down_last = scatter_about(key_of[14], (FF, D), FF ** -0.5, 0.078125, ((0, 4), (1, 4)))
    return dict(tokens=tokens, gain_first=gain_first, gate_first=gate_first, up_first=up_first, down_first=down_first, gain_mixer=gain_mixer, outer_gate=outer_gate, inner_gate=inner_gate, conv_input=conv_input, conv_taps=conv_taps, mixer_out=mixer_out, gain_last=gain_last, gate_last=gate_last, up_last=up_last, down_last=down_last)


norm_eps = 1e-06

def rms_rows(residual, gain_vec):
    inverse = lax.rsqrt(lax.optimization_barrier(jnp.mean(residual * residual, axis=1, keepdims=True)) + norm_eps)
    return (residual * inverse * gain_vec).astype(jnp.bfloat16)

def blocked_sum(left_rows, right_rows):
    extent = left_rows.shape[1] // N_TP
    running = jnp.zeros((left_rows.shape[0], right_rows.shape[1]), jnp.float32)
    for block_id in range(N_TP):
        branch = jnp.dot(left_rows[:, block_id * extent:(block_id + 1) * extent], right_rows[block_id * extent:(block_id + 1) * extent], preferred_element_type=jnp.float32).astype(jnp.bfloat16)
        running = running + lax.optimization_barrier(branch).astype(jnp.float32)
    return running

def causal_mixing(gated, conv_taps):
    row_count, channels = gated.shape
    shaped = gated.reshape(row_count // SEQ_LEN, SEQ_LEN, channels)
    kernel = conv_taps.shape[0]
    padded = jnp.pad(shaped, ((0, 0), (kernel - 1, 0), (0, 0)))
    result = jnp.zeros_like(shaped)
    for offset in range(kernel):
        result = result + conv_taps[offset] * padded[:, offset:offset + SEQ_LEN]
    return result.reshape(row_count, channels)

def half_step(residual, gain_vec, gate_weight, up_weight, down_weight):
    normed = rms_rows(residual, gain_vec)
    gate_pre = jnp.dot(normed, gate_weight, preferred_element_type=jnp.float32)
    up_pre = jnp.dot(normed, up_weight, preferred_element_type=jnp.float32)
    hidden = (jax.nn.silu(gate_pre) * up_pre).astype(jnp.bfloat16)
    return residual + 0.5 * blocked_sum(hidden, down_weight)

def reference(tokens, gain_first, gate_first, up_first, down_first, gain_mixer, outer_gate, inner_gate, conv_input, conv_taps, mixer_out, gain_last, gate_last, up_last, down_last):
    residual = tokens.astype(jnp.float32)
    residual = half_step(residual, gain_first, gate_first, up_first, down_first)
    normed = rms_rows(residual, gain_mixer)
    outer_pre = jnp.dot(normed, outer_gate, preferred_element_type=jnp.float32)
    inner_pre = jnp.dot(normed, inner_gate, preferred_element_type=jnp.float32)
    value_pre = jnp.dot(normed, conv_input, preferred_element_type=jnp.float32)
    convolved = causal_mixing(inner_pre * value_pre, conv_taps)
    mixed_rows = (outer_pre * convolved).astype(jnp.bfloat16)
    residual = residual + blocked_sum(mixed_rows, mixer_out)
    residual = half_step(residual, gain_last, gate_last, up_last, down_last)
    return residual.astype(jnp.bfloat16)
```

```python
import functools

import jax
import jax.numpy as jnp
from jax import lax
from jax.experimental import pallas as pl
from jax.experimental.pallas import tpu as pltpu
from jax.sharding import PartitionSpec as P

SEQ_LEN = 64
NORM_EPS = 1e-06
CORES = 2


bf16 = jnp.bfloat16
f32 = jnp.float32


def row_block(rows):
    for parts in (3, 2, 4, 1):
        if rows % (parts * SEQ_LEN) == 0:
            return rows // parts
    return rows


def whole(array):
    rank = len(array.shape)
    return pl.BlockSpec(array.shape, lambda i, *_: (0,) * rank)


def row_spec(block, cols):
    return pl.BlockSpec((block, cols), lambda i, *_: (i, 0))


def store_normed(cols_ref, pieces, gain_ref, normed_ref, width):
    total = None
    for piece in pieces:
        value = piece[...].astype(f32)
        part = jnp.sum(value * value, axis=1, keepdims=True)
        total = part if total is None else total + part
    inverse = lax.rsqrt(total / (width * len(pieces)) + NORM_EPS)
    for index, piece in enumerate(pieces):
        start = pl.multiple_of(cols_ref[index], width)
        value = piece[...].astype(f32) * inverse * gain_ref[:, pl.ds(start, width)]
        normed_ref[:, pl.ds(start, width)] = value.astype(bf16)


def project(cols_ref, first, normed_ref, weights, part):
    total = None
    for index, weight in enumerate(weights):
        depth = weight.shape[-2]
        start = pl.multiple_of(cols_ref[first + index], depth)
        rows = normed_ref[:, pl.ds(start, depth)]
        value = jnp.dot(rows, weight[part], preferred_element_type=f32)
        total = value if total is None else total + value
    return total


def store_split(cols_ref, first, rows, weights, out_nat, keep_ref, send_ref, core, blocks):
    for index, weight in enumerate(weights):
        width = weight.shape[-1]
        start = pl.multiple_of(cols_ref[first + index], width)
        value = jnp.dot(rows, weight[...], preferred_element_type=f32)
        out_nat[:, pl.ds(start, width)] = value.astype(bf16)
    width = keep_ref.shape[-1] // blocks
    for block in range(blocks):
        mine = pl.multiple_of((block * CORES + core) * width, width)
        other = pl.multiple_of((block * CORES + (CORES - 1) - core) * width, width)
        keep_ref[:, block * width : (block + 1) * width] = out_nat[:, pl.ds(mine, width)]
        send_ref[:, block * width : (block + 1) * width] = out_nat[:, pl.ds(other, width)]


def gated_kernel(n_pieces, n_weights, cols_ref, gain_ref, *refs):
    pieces, weights = refs[:n_pieces], refs[n_pieces : n_pieces + 2 * n_weights]
    out_ref, normed_ref = refs[n_pieces + 2 * n_weights :]
    store_normed(cols_ref, pieces, gain_ref, normed_ref, pieces[0].shape[-1])
    gate = project(cols_ref, n_pieces, normed_ref, weights[:n_weights], slice(None))
    up = project(cols_ref, n_pieces, normed_ref, weights[n_weights:], slice(None))
    out_ref[...] = (gate / (1.0 + jnp.exp(-gate)) * up).astype(bf16)


def gated_call(cols, gain, pieces, gates, ups):
    rows, width = pieces[0].shape
    block = row_block(rows)
    hidden = gates[0].shape[-1]
    features = width * len(pieces)
    specs = [pl.BlockSpec(gain.shape, lambda i, *_: (0, 0))]
    specs += [row_spec(block, width)] * len(pieces)
    specs += [whole(w) for w in (*gates, *ups)]
    return pl.pallas_call(
        functools.partial(gated_kernel, len(pieces), len(gates)),
        grid_spec=pltpu.PrefetchScalarGridSpec(
            num_scalar_prefetch=1,
            grid=(rows // block,),
            in_specs=specs,
            out_specs=row_spec(block, hidden),
            scratch_shapes=[pltpu.VMEM((block, features), bf16)],
        ),
        out_shape=jax.ShapeDtypeStruct((rows, hidden), bf16),
        compiler_params=pltpu.CompilerParams(dimension_semantics=("arbitrary",)),
        cost_estimate=pl.CostEstimate(
            flops=4 * rows * features * hidden,
            transcendentals=rows * hidden,
            bytes_accessed=2 * (rows * features + 2 * features * hidden + rows * hidden),
        ),
        name="gated",
    )(cols, gain, *pieces, *gates, *ups)


def down_kernel(n_weights, blocks, cols_ref, hidden_ref, *refs):
    weights = refs[:n_weights]
    keep_ref, send_ref, out_nat = refs[n_weights:]
    store_split(cols_ref, 1, hidden_ref[...], weights, out_nat, keep_ref, send_ref, cols_ref[0], blocks)


def down_call(cols, hidden, weights, blocks):
    rows, depth = hidden.shape
    block = row_block(rows)
    features = sum(w.shape[-1] for w in weights)
    half = features // CORES
    return pl.pallas_call(
        functools.partial(down_kernel, len(weights), blocks),
        grid_spec=pltpu.PrefetchScalarGridSpec(
            num_scalar_prefetch=1,
            grid=(rows // block,),
            in_specs=[row_spec(block, depth)] + [whole(w) for w in weights],
            out_specs=[row_spec(block, half)] * 2,
            scratch_shapes=[pltpu.VMEM((block, features), bf16)],
        ),
        out_shape=[jax.ShapeDtypeStruct((rows, half), bf16)] * 2,
        compiler_params=pltpu.CompilerParams(dimension_semantics=("arbitrary",)),
        cost_estimate=pl.CostEstimate(
            flops=2 * rows * features * depth,
            transcendentals=0,
            bytes_accessed=2 * (rows * features + features * depth + rows * depth),
        ),
        name="down",
    )(cols, hidden, *weights)


def shifted_rows(value, amount, position):
    if amount == 0:
        return value
    moved = pltpu.roll(value, amount, 0)
    return jnp.where(position >= amount, moved, 0.0)


def mixer_kernel(n_pieces, n_weights, blocks, cols_ref, gain_ref, taps_ref, *refs):
    pieces = refs[:n_pieces]
    inputs = refs[n_pieces : n_pieces + n_weights]
    outs = refs[n_pieces + n_weights : n_pieces + 2 * n_weights]
    keep_ref, send_ref, normed_ref, out_nat = refs[n_pieces + 2 * n_weights :]
    store_normed(cols_ref, pieces, gain_ref, normed_ref, pieces[0].shape[-1])
    first = n_pieces + 1
    outer = project(cols_ref, first, normed_ref, inputs, 0)
    inner = project(cols_ref, first, normed_ref, inputs, 1)
    value = project(cols_ref, first, normed_ref, inputs, 2)
    gated = inner * value
    position = lax.broadcasted_iota(jnp.int32, gated.shape, 0) % SEQ_LEN
    kernel = taps_ref.shape[0]
    convolved = None
    for tap in range(kernel):
        part = taps_ref[tap : tap + 1, :] * shifted_rows(gated, kernel - 1 - tap, position)
        convolved = part if convolved is None else convolved + part
    mixed = (outer * convolved).astype(bf16)
    store_split(
        cols_ref, first + n_weights, mixed, outs, out_nat, keep_ref, send_ref, cols_ref[n_pieces], blocks
    )


def mixer_call(cols, gain, taps, pieces, inputs, outs, blocks):
    rows, width = pieces[0].shape
    block = row_block(rows)
    features = width * len(pieces)
    half = features // CORES
    channels = taps.shape[-1]
    specs = [pl.BlockSpec(gain.shape, lambda i, *_: (0, 0)), whole(taps)]
    specs += [row_spec(block, width)] * len(pieces)
    specs += [whole(w) for w in (*inputs, *outs)]
    return pl.pallas_call(
        functools.partial(mixer_kernel, len(pieces), len(inputs), blocks),
        grid_spec=pltpu.PrefetchScalarGridSpec(
            num_scalar_prefetch=1,
            grid=(rows // block,),
            in_specs=specs,
            out_specs=[row_spec(block, half)] * 2,
            scratch_shapes=[pltpu.VMEM((block, features), bf16)] * 2,
        ),
        out_shape=[jax.ShapeDtypeStruct((rows, half), bf16)] * 2,
        compiler_params=pltpu.CompilerParams(dimension_semantics=("arbitrary",)),
        cost_estimate=pl.CostEstimate(
            flops=8 * rows * features * channels,
            transcendentals=0,
            bytes_accessed=2 * (2 * rows * features + 4 * features * channels),
        ),
        name="mixer",
    )(cols, gain, taps, *pieces, *inputs, *outs)


def shards(n_grp, n_fs, n_tp, *args):
    (
        tokens,
        gain_first,
        gate_first,
        up_first,
        down_first,
        gain_mixer,
        outer_gate,
        inner_gate,
        conv_input,
        conv_taps,
        mixer_out,
        gain_last,
        gate_last,
        up_last,
        down_last,
    ) = args
    rows, width = tokens.shape
    n_x = n_tp // CORES
    grp, fs, tp = (lax.axis_index(name) for name in ("grp", "fs", "tp"))
    x_index, core = tp // CORES, tp % CORES
    relayed = n_fs == 4

    def own_half(array, axis):
        extent = array.shape[axis] // n_grp
        return lax.dynamic_slice_in_dim(array, grp * extent, extent, axis)

    def fs_shift(array, offset):
        return lax.ppermute(array, "fs", [(i, (i + offset) % n_fs) for i in range(n_fs)])

    sources = [fs] + [(fs - offset) % n_fs for offset in range(1, n_fs)]

    def spread_near(array, after):
        if after is not None:
            array, _ = lax.optimization_barrier((array, after))
        return [array] + [fs_shift(array, offset) for offset in range(1, n_fs) if not (relayed and offset == 2)]

    def spread_far(near):
        if not relayed:
            return near, near[0]
        own, below, above = near
        load = jnp.where(fs == 1, above, jnp.where(fs == 2, below, own))
        far = lax.ppermute(load, "fs", [(3, 1), (0, 2), (1, 0), (2, 3)])
        return [own, below, far, above], load

    ready = [
        own_half(gate_first, 1),
        own_half(up_first, 1),
        own_half(down_first, 0),
        jnp.stack([own_half(w, 1) for w in (outer_gate, inner_gate, conv_input)]),
        own_half(mixer_out, 0),
        own_half(gate_last, 1),
        own_half(up_last, 1),
        own_half(down_last, 0),
    ]
    gathered, loads = [], []
    for index, array in enumerate(ready):
        near = spread_near(array, loads[index - 2] if index >= 2 else None)
        full, load = spread_far(near)
        gathered.append(full)
        loads.append(load)

    def tp_shift(array, offset):
        return lax.ppermute(
            array,
            "tp",
            [(x * CORES + c, (x - offset) % n_x * CORES + c) for x in range(n_x) for c in range(CORES)],
        )

    def core_swap(array):
        return lax.ppermute(array, "tp", [(t, t ^ 1) for t in range(n_tp)])

    def gather_rows(own):
        parts = [own]
        for offset in range(1, n_grp):
            parts.append(lax.ppermute(own, "grp", [((i + offset) % n_grp, i) for i in range(n_grp)]))
        block = jnp.concatenate(parts, axis=0)
        pieces = [block, core_swap(block)]
        for offset in range(1, n_x):
            moved = tp_shift(block, offset)
            pieces += [moved, core_swap(moved)]
        return pieces

    piece_index = []
    for offset in range(n_x):
        owner = (x_index + offset) % n_x * CORES
        piece_index += [owner + core, owner + (CORES - 1) - core]
    piece_cols = jnp.stack(piece_index).astype(jnp.int32) * width
    depth_cols = jnp.stack(sources).astype(jnp.int32) * (width * n_tp // n_fs)
    core_scalar = core.astype(jnp.int32)[None]

    def sum_rows(keep, send):
        got = core_swap(send)

        def columns(array, index):
            return lax.dynamic_slice_in_dim(array, index * width, width, 1).astype(f32)

        total = columns(keep, x_index) + columns(got, x_index)
        for offset in range(1, n_x):
            target = (x_index - offset) % n_x
            out = (columns(keep, target) + columns(got, target)).astype(bf16)
            total = total + tp_shift(out, offset).astype(f32)
        result = total[:rows]
        for offset in range(1, n_grp):
            out = total[offset * rows : (offset + 1) * rows].astype(bf16)
            got_rows = lax.ppermute(out, "grp", [(i, (i + offset) % n_grp) for i in range(n_grp)])
            result = result + got_rows.astype(f32)
        return result

    gated_cols = jnp.concatenate([piece_cols, depth_cols])
    down_cols = jnp.concatenate([core_scalar, depth_cols])
    mixer_cols = jnp.concatenate([piece_cols, core_scalar, depth_cols, depth_cols])

    def half_step(residual, own, gain, gates, ups, downs):
        hidden = gated_call(gated_cols, gain[None], gather_rows(own), gates, ups)
        keep, send = down_call(down_cols, hidden, downs, n_x)
        return residual + 0.5 * sum_rows(keep, send)

    residual = half_step(tokens.astype(f32), tokens, gain_first, *gathered[:3])
    keep, send = mixer_call(
        mixer_cols,
        gain_mixer[None],
        own_half(conv_taps, 1),
        gather_rows(residual.astype(bf16)),
        gathered[3],
        gathered[4],
        n_x,
    )
    residual = residual + sum_rows(keep, send)
    residual = half_step(residual, residual.astype(bf16), gain_last, *gathered[5:])
    return residual.astype(bf16)


def solution(mesh):
    in_specs = (
        P(("grp", "fs"), "tp"),
        P(),
        P("fs", "tp"),
        P("fs", "tp"),
        P("tp", "fs"),
        P(),
        P("fs", "tp"),
        P("fs", "tp"),
        P("fs", "tp"),
        P(None, "tp"),
        P("tp", "fs"),
        P(),
        P("fs", "tp"),
        P("fs", "tp"),
        P("tp", "fs"),
    )
    body = functools.partial(shards, *(mesh.shape[name] for name in ("grp", "fs", "tp")))
    return jax.shard_map(
        body, mesh=mesh, in_specs=in_specs, out_specs=P(("grp", "fs"), "tp"), check_vma=False
    )
```

```python
import functools

import jax
import jax.numpy as jnp
from jax import lax
from jax.experimental import pallas as pl
from jax.experimental.pallas import tpu as pltpu
from jax.sharding import PartitionSpec as P


SEQ_LEN = 64
NORM_EPS = 1e-06
CORES = 2


bf16 = jnp.bfloat16
f32 = jnp.float32


def row_block(rows):
    for parts in (2, 1):
        if rows % (parts * SEQ_LEN) == 0:
            return rows // parts
    return rows


def whole(array):
    rank = len(array.shape)
    return pl.BlockSpec(array.shape, lambda i, *_: (0,) * rank)


def row_spec(block, cols):
    return pl.BlockSpec((block, cols), lambda i, *_: (i, 0))


def store_normed(cols_ref, groups, gain_ref, normed_ref):
    step = pl.program_id(0)
    block = normed_ref.shape[0]
    steps = groups[0][0].shape[0] // block
    width = groups[0][0].shape[1]
    for group, pieces in enumerate(groups):

        @pl.when(step // steps == group)
        def _(pieces=pieces):
            rows = pl.ds(pl.multiple_of(step % steps * block, block), block)
            total = None
            for piece in pieces:
                value = piece[rows, :].astype(f32)
                part = jnp.sum(value * value, axis=1, keepdims=True)
                total = part if total is None else total + part
            inverse = lax.rsqrt(total / (width * len(pieces)) + NORM_EPS)
            for index, piece in enumerate(pieces):
                start = pl.multiple_of(cols_ref[index], width)
                value = piece[rows, :].astype(f32) * inverse * gain_ref[:, pl.ds(start, width)]
                normed_ref[:, pl.ds(start, width)] = value.astype(bf16)


def project(cols_ref, first, normed_ref, weights):
    total = None
    for index, weight in enumerate(weights):
        depth = weight.shape[0]
        start = pl.multiple_of(cols_ref[first + index], depth)
        rows = normed_ref[:, pl.ds(start, depth)]
        value = jnp.dot(rows, weight[...], preferred_element_type=f32)
        total = value if total is None else total + value
    return total


def store_split(cols_ref, first, rows, weights, out_nat, keep_ref, send_ref, core, blocks):
    for index, weight in enumerate(weights):
        width = weight.shape[-1]
        start = pl.multiple_of(cols_ref[first + index], width)
        value = jnp.dot(rows, weight[...], preferred_element_type=f32)
        out_nat[:, pl.ds(start, width)] = value.astype(bf16)
    width = keep_ref.shape[-1] // blocks
    for block in range(blocks):
        mine = pl.multiple_of((block * CORES + core) * width, width)
        other = pl.multiple_of((block * CORES + (CORES - 1) - core) * width, width)
        keep_ref[:, block * width : (block + 1) * width] = out_nat[:, pl.ds(mine, width)]
        send_ref[:, block * width : (block + 1) * width] = out_nat[:, pl.ds(other, width)]


def regroup(pieces, n_groups):
    size = len(pieces) // n_groups
    return [pieces[g * size : (g + 1) * size] for g in range(n_groups)]


def gated_kernel(n_groups, n_pieces, n_weights, cols_ref, gain_ref, *refs):
    groups, weights = regroup(refs[:n_pieces], n_groups), refs[n_pieces : n_pieces + 2 * n_weights]
    out_ref, normed_ref = refs[n_pieces + 2 * n_weights :]
    store_normed(cols_ref, groups, gain_ref, normed_ref)
    first = n_pieces // n_groups
    gate = project(cols_ref, first, normed_ref, weights[:n_weights])
    up = project(cols_ref, first, normed_ref, weights[n_weights:])
    out_ref[...] = (gate / (1.0 + jnp.exp(-gate)) * up).astype(bf16)


def gated_call(cols, gain, groups, gates, ups):
    rows, width = groups[0][0].shape
    pieces = [piece for group in groups for piece in group]
    block = row_block(rows)
    rows = rows * len(groups)
    hidden = gates[0].shape[-1]
    features = width * len(groups[0])
    inputs = [gain, *pieces, *gates, *ups]
    return pl.pallas_call(
        functools.partial(gated_kernel, len(groups), len(pieces), len(gates)),
        grid_spec=pltpu.PrefetchScalarGridSpec(
            num_scalar_prefetch=1,
            grid=(rows // block,),
            in_specs=[whole(array) for array in inputs],
            out_specs=row_spec(block, hidden),
            scratch_shapes=[pltpu.VMEM((block, features), bf16)],
        ),
        out_shape=jax.ShapeDtypeStruct((rows, hidden), bf16),
        compiler_params=pltpu.CompilerParams(dimension_semantics=("arbitrary",)),
        cost_estimate=pl.CostEstimate(
            flops=4 * rows * features * hidden,
            transcendentals=rows * hidden,
            bytes_accessed=2 * (rows * features + 2 * features * hidden + rows * hidden),
        ),
        name="gated",
    )(cols, *inputs)


def down_kernel(n_weights, blocks, cols_ref, hidden_ref, *refs):
    weights = refs[:n_weights]
    keep_ref, send_ref, out_nat = refs[n_weights:]
    store_split(cols_ref, 1, hidden_ref[...], weights, out_nat, keep_ref, send_ref, cols_ref[0], blocks)


def down_call(cols, hidden, weights, blocks):
    rows, depth = hidden.shape
    block = row_block(rows)
    features = sum(w.shape[-1] for w in weights)
    half = features // CORES
    return pl.pallas_call(
        functools.partial(down_kernel, len(weights), blocks),
        grid_spec=pltpu.PrefetchScalarGridSpec(
            num_scalar_prefetch=1,
            grid=(rows // block,),
            in_specs=[row_spec(block, depth)] + [whole(w) for w in weights],
            out_specs=[row_spec(block, half)] * 2,
            scratch_shapes=[pltpu.VMEM((block, features), bf16)],
        ),
        out_shape=[jax.ShapeDtypeStruct((rows, half), bf16)] * 2,
        compiler_params=pltpu.CompilerParams(dimension_semantics=("arbitrary",)),
        cost_estimate=pl.CostEstimate(
            flops=2 * rows * features * depth,
            transcendentals=0,
            bytes_accessed=2 * (rows * features + features * depth + rows * depth),
        ),
        name="down",
    )(cols, hidden, *weights)


def shifted_rows(value, amount, position):
    if amount == 0:
        return value
    moved = pltpu.roll(value, amount, 0)
    return jnp.where(position >= amount, moved, 0.0)


def mixer_kernel(n_groups, n_pieces, n_weights, blocks, cols_ref, gain_ref, taps_ref, *refs):
    groups = regroup(refs[:n_pieces], n_groups)
    inputs = refs[n_pieces : n_pieces + n_weights]
    outs = refs[n_pieces + n_weights : n_pieces + 2 * n_weights]
    keep_ref, send_ref, normed_ref, out_nat = refs[n_pieces + 2 * n_weights :]
    store_normed(cols_ref, groups, gain_ref, normed_ref)
    first = n_pieces // n_groups
    core = cols_ref[first]
    joined = project(cols_ref, first + 1, normed_ref, inputs)
    channels = taps_ref.shape[1]
    outer, inner, value = (joined[:, i * channels : (i + 1) * channels] for i in range(3))
    gated = inner * value
    position = lax.broadcasted_iota(jnp.int32, gated.shape, 0) % SEQ_LEN
    kernel = taps_ref.shape[0]
    convolved = None
    for tap in range(kernel):
        part = taps_ref[tap : tap + 1, :] * shifted_rows(gated, kernel - 1 - tap, position)
        convolved = part if convolved is None else convolved + part
    mixed = (outer * convolved).astype(bf16)
    store_split(cols_ref, first + 1 + n_weights, mixed, outs, out_nat, keep_ref, send_ref, core, blocks)


def mixer_call(cols, gain, taps, groups, inputs, outs, blocks):
    rows, width = groups[0][0].shape
    pieces = [piece for group in groups for piece in group]
    block = row_block(rows)
    rows = rows * len(groups)
    features = width * len(groups[0])
    half = features // CORES
    channels = taps.shape[-1]
    arrays = [gain, taps, *pieces, *inputs, *outs]
    return pl.pallas_call(
        functools.partial(mixer_kernel, len(groups), len(pieces), len(inputs), blocks),
        grid_spec=pltpu.PrefetchScalarGridSpec(
            num_scalar_prefetch=1,
            grid=(rows // block,),
            in_specs=[whole(array) for array in arrays],
            out_specs=[row_spec(block, half)] * 2,
            scratch_shapes=[pltpu.VMEM((block, features), bf16)] * 2,
        ),
        out_shape=[jax.ShapeDtypeStruct((rows, half), bf16)] * 2,
        compiler_params=pltpu.CompilerParams(dimension_semantics=("arbitrary",)),
        cost_estimate=pl.CostEstimate(
            flops=8 * rows * features * channels,
            transcendentals=0,
            bytes_accessed=2 * (2 * rows * features + 4 * features * channels),
        ),
        name="mixer",
    )(cols, *arrays)


def relays(n_fs):
    return n_fs == 4


def last_parts(n_fs, n_tp):
    return 2 if relays(n_fs) and n_fs == n_tp else 1


def shards(n_grp, n_fs, n_tp, *args):
    return layer(n_grp, n_fs, n_tp, *args)


def layer(n_grp, n_fs, n_tp, *args):
    (
        tokens,
        gain_first,
        gate_first,
        up_first,
        down_first,
        gain_mixer,
        outer_gate,
        inner_gate,
        conv_input,
        conv_taps,
        mixer_out,
        gain_last,
        gate_last,
        up_last,
        down_last,
    ) = args
    rows, width = tokens.shape
    n_x = n_tp // CORES
    grp, fs, tp = (lax.axis_index(name) for name in ("grp", "fs", "tp"))
    x_index, core = tp // CORES, tp % CORES

    def own_half(array, axis):
        extent = array.shape[axis] // n_grp
        return lax.dynamic_slice_in_dim(array, grp * extent, extent, axis)

    sources = [fs] + [(fs - offset) % n_fs for offset in range(1, n_fs)]

    def spread(own):
        def shift(offset):
            perm = [(i, (i + offset) % n_fs) for i in range(n_fs)]
            return lax.ppermute(own, "fs", perm)

        if not relays(n_fs):
            return [own] + [shift(offset) for offset in range(1, n_fs)]
        below, above = shift(1), shift(3)
        load = jnp.where(fs == 1, above, jnp.where(fs == 2, below, own))
        far = lax.ppermute(load, "fs", [(3, 1), (0, 2), (1, 0), (2, 3)])
        return [own, below, far, above]

    ready = [
        own_half(gate_first, 1),
        own_half(up_first, 1),
        own_half(down_first, 0),
        jnp.concatenate([own_half(w, 1) for w in (outer_gate, inner_gate, conv_input)], axis=1),
        own_half(mixer_out, 0),
        own_half(gate_last, 1),
        own_half(up_last, 1),
    ]
    parts = last_parts(n_fs, n_tp)
    cut = down_last.shape[1] // parts
    last = own_half(down_last, 0)
    ready += [last[:, part * cut : (part + 1) * cut] for part in range(parts)]
    gathered = [spread(array) for array in ready]

    places = [(g, x) for g in range(n_grp) for x in range(n_x)]

    def place_perm(g_off, x_off):
        pairs = []
        for g in range(n_grp):
            for t in range(n_tp):
                to = (t // CORES + x_off) % n_x * CORES + t % CORES
                pairs.append((g * n_tp + t, (g + g_off) % n_grp * n_tp + to))
        return pairs

    def core_swap(array):
        return lax.ppermute(array, "tp", [(t, t ^ 1) for t in range(n_tp)])

    def gather_rows(own):
        groups = [[] for _ in range(n_grp)]
        for g, x in places:
            piece = own
            if (g, x) != (0, 0):
                piece = lax.ppermute(own, ("grp", "tp"), place_perm(-g, -x))
            groups[g] += [piece, core_swap(piece)]
        return groups

    piece_index = []
    for offset in range(n_x):
        owner = (x_index + offset) % n_x * CORES
        piece_index += [owner + core, owner + (CORES - 1) - core]
    piece_cols = jnp.stack(piece_index).astype(jnp.int32) * width
    source_index = jnp.stack(sources).astype(jnp.int32)
    depth_cols = source_index * (width * n_tp // n_fs)
    core_scalar = core.astype(jnp.int32)[None]

    def sum_rows(keep, send):
        got = core_swap(send)
        cols = keep.shape[1] // n_x

        def block(g, x):
            start = (g * rows, (x_index + x) % n_x * cols)
            addends = (lax.dynamic_slice(array, start, (rows, cols)) for array in (keep, got))
            return sum(addend.astype(f32) for addend in addends)

        total = block(0, 0)
        for g, x in places[1:]:
            moved = lax.ppermute(block(g, x).astype(bf16), ("grp", "tp"), place_perm(g, x))
            total = total + moved.astype(f32)
        return total

    gated_cols = jnp.concatenate([piece_cols, depth_cols])
    mixer_cols = jnp.concatenate([piece_cols, core_scalar, depth_cols, depth_cols])

    def half_step(residual, own, gain, gates, ups, downs):
        pieces = gather_rows(own)
        hidden = gated_call(gated_cols, gain[None], pieces, gates, ups)
        out, start = [], 0
        for weights in downs:
            cols = jnp.concatenate([core_scalar, source_index * weights[0].shape[1]])
            keep, send = down_call(cols, hidden, weights, n_x)
            branch = sum_rows(keep, send)
            out.append(residual[:, start : start + branch.shape[1]] + 0.5 * branch)
            start += branch.shape[1]
        return out[0] if len(out) == 1 else jnp.concatenate(out, axis=1)

    residual = half_step(tokens.astype(f32), tokens, gain_first, *gathered[:2], gathered[2:3])
    keep, send = mixer_call(
        mixer_cols,
        gain_mixer[None],
        own_half(conv_taps, 1),
        gather_rows(residual.astype(bf16)),
        gathered[3],
        gathered[4],
        n_x,
    )
    residual = residual + sum_rows(keep, send)
    residual = half_step(residual, residual.astype(bf16), gain_last, *gathered[5:7], gathered[7:])
    return residual.astype(bf16)


def solution(mesh):
    in_specs = (
        P(("grp", "fs"), "tp"),
        P(),
        P("fs", "tp"),
        P("fs", "tp"),
        P("tp", "fs"),
        P(),
        P("fs", "tp"),
        P("fs", "tp"),
        P("fs", "tp"),
        P(None, "tp"),
        P("tp", "fs"),
        P(),
        P("fs", "tp"),
        P("fs", "tp"),
        P("tp", "fs"),
    )
    n_grp, n_fs, n_tp = (mesh.shape[name] for name in ("grp", "fs", "tp"))
    body = functools.partial(shards, n_grp, n_fs, n_tp)
    step = jax.shard_map(
        body, mesh=mesh, in_specs=in_specs, out_specs=P(("grp", "fs"), "tp"), check_vma=False
    )
    if last_parts(n_fs, n_tp) != 2:
        return step
    return step
```
